32 devices in a mesh: ra: 4 (over z), cb: 4 (over y, x), dp: 2 (over core).
Axes of the slice: x: 2, y: 2, z: 4, core: 2. Of those that a mesh axis runs over, the one named last changes fastest.
Arguments:
- tokens: bfloat16 [2048, 4096], P('dp', 'cb'), may hold values from -3000 to 3000
- norm_gain: float32 [4096], P('cb'), may hold values from 0.1 to 1.9
- norm_bias: float32 [4096], P('cb'), may hold values from -2 to 2
- gate_weight: float32 [4096, 11264], P('cb', 'ra'), may hold values from -0.09375 to 0.09375
- up_weight: float32 [4096, 11264], P('cb', 'ra'), may hold values from -0.09375 to 0.09375
- gate_scale: float32 [11264], P('ra'), may hold values from 0.5 to 2
- up_scale: float32 [11264], P('ra'), may hold values from 0.5 to 2
- down_weight: float32 [11264, 4096], P('ra', 'cb'), may hold values from -0.0546875 to 0.0546875
- down_scale: float32 [4096], P('cb'), may hold values from 0.5 to 8
- out_gain: float32 [4096], P('cb'), may hold values from 0.1 to 1.9
- out_bias: float32 [4096], P('cb'), may hold values from -2 to 2
Outputs:
- result: bfloat16 [2048, 4096], P(('dp', 'ra'), 'cb')
The draws below stay inside these ranges and needn't reach their ends.
All inputs are finite; a program needn't handle non-finite values.
Results may differ from the reference program's by a relative error of at most 0.018.
Values may be sent and summed in bfloat16 or wider, within the bound.
A program may use at most 128 MiB of HBM per device.

```python
import math
import jax
import jax.numpy as jnp
from jax import lax

D = 4096
FF = 11264
TOKENS = 2048


def draw_tokens(key, part):
    keys = jax.random.split(key, 3)
    base = jax.random.normal(keys[0], (TOKENS, D), jnp.float32)
    columns = jnp.exp(math.log(6.0) * jnp.arange(D, dtype=jnp.float32) / D)
    columns = columns * jnp.exp(jax.random.uniform(keys[1], (D,), jnp.float32, -0.35, 0.35))
    rows_scale = jnp.exp(jax.random.uniform(keys[2], (TOKENS, 1), jnp.float32, 0.0, math.log(10.0)))
    values = base * columns * rows_scale
    return values.astype(jnp.bfloat16)


def draw_down_scale(key, part):
    rising = jnp.exp(math.log(4.0) * jnp.arange(D, dtype=jnp.float32) / D)
    factor = jnp.exp(jax.random.uniform(key, (D,), jnp.float32, math.log(0.5), math.log(2.0)))
    return (rising * factor).astype(jnp.float32)


def level_of(own_key, extent, pieces, smallest, high):
    def one(dim, shards_of):
        heights = jax.random.uniform(jax.random.fold_in(jax.random.fold_in(own_key, 6), dim), (shards_of,), jnp.float32, smallest / len(pieces), high / len(pieces))
        return jnp.repeat(jnp.exp(heights), extent[dim] // shards_of).reshape((-1,) + (1,) * (len(extent) - dim - 1))

    gain = one(*pieces[0])
    for cut in pieces[1:]:
        gain = gain * one(*cut)
    return gain


def gaussian(stream_key, dims, deviation, limit, pieces=(), kind=jnp.bfloat16):
    result = jax.random.normal(stream_key, dims, jnp.float32) * deviation
    if len(pieces) > 0:
        result = level_of(stream_key, dims, pieces, -0.22, 0.18) * result
    return jnp.clip(result, min=-limit, max=limit).astype(kind)


def setup_inputs(seed: int = 0) -> dict:
    streams_of = jax.random.split(jax.random.key(seed), 12)
    tokens = draw_tokens(jax.random.fold_in(streams_of[11], 71), 0)
    norm_gain = jnp.clip(1.0 + 0.18 * jax.random.normal(streams_of[1], (D,), jnp.float32), 0.1, 1.9)
    norm_bias = gaussian(streams_of[2], (D,), 0.3, 2.0, ((0, 4),), jnp.float32)
    gate_weight = gaussian(streams_of[3], (D, FF), D ** -0.5, 0.09375, ((0, 4), (1, 4)), jnp.float32)
    up_weight = gaussian(streams_of[4], (D, FF), D ** -0.5, 0.09375, ((0, 4), (1, 4)), jnp.float32)
    gate_scale = jnp.clip(jnp.exp(math.log(2.0) - 1.3862944 * jax.random.uniform(streams_of[5], (FF,), jnp.float32) ** level_of(streams_of[5], (FF,), ((0, 4),), -0.2, 0.2)), 0.5, 2.0)
    up_scale = jnp.clip(jnp.exp(math.log(2.0) - 1.3862944 * jax.random.uniform(streams_of[6], (FF,), jnp.float32) ** level_of(streams_of[6], (FF,), ((0, 4),), -0.2, 0.2)), 0.5, 2.0)
    down_weight = gaussian(streams_of[7], (FF, D), FF ** -0.5, 0.0546875, ((0, 4), (1, 4)), jnp.float32)
    down_scale = draw_down_scale(jax.random.fold_in(streams_of[11], 71), 0)
    out_gain = jnp.clip(1.0 + 0.18 * jax.random.normal(streams_of[9], (D,), jnp.float32), 0.1, 1.9)
    out_bias = gaussian(streams_of[10], (D,), 0.3, 2.0, ((0, 4),), jnp.float32)
    return dict(tokens=tokens, norm_gain=norm_gain, norm_bias=norm_bias, gate_weight=gate_weight, up_weight=up_weight, gate_scale=gate_scale, up_scale=up_scale, down_weight=down_weight, down_scale=down_scale, out_gain=out_gain, out_bias=out_bias)


def standardize(values):
    mean = lax.optimization_barrier(jnp.mean(values, axis=1, keepdims=True))
    centred = values - mean
    spread = lax.optimization_barrier(jnp.mean(centred * centred, axis=1, keepdims=True))
    return centred * lax.rsqrt(spread + 1e-05)

def reference(tokens, norm_gain, norm_bias, gate_weight, up_weight, gate_scale, up_scale, down_weight, down_scale, out_gain, out_bias):
    normed = (standardize(tokens.astype(jnp.float32)) * norm_gain + norm_bias).astype(jnp.bfloat16)
    gate = jnp.dot(normed, gate_weight.astype(jnp.bfloat16), preferred_element_type=jnp.float32) * gate_scale
    up = jnp.dot(normed, up_weight.astype(jnp.bfloat16), preferred_element_type=jnp.float32) * up_scale
    hidden = (jax.nn.silu(gate) * up).astype(jnp.bfloat16)
    branch = jnp.dot(hidden, down_weight.astype(jnp.bfloat16), preferred_element_type=jnp.float32) * down_scale
    mixed = 0.5 * normed.astype(jnp.float32) + branch
    return (standardize(mixed) * out_gain + out_bias).astype(jnp.bfloat16)
```

```python
import jax
import jax.numpy as jnp
from jax import lax
from jax.experimental import pallas as pl
from jax.experimental.pallas import tpu as pltpu
from jax.sharding import PartitionSpec as P

MESH = pl.DeviceIdType.MESH
EPS = 1e-05
TILE = 256
G = 4
F32 = jnp.float32
BF16 = jnp.bfloat16


def standardize(values):
    width = values.shape[1] * lax.axis_size("cb")
    total = lax.psum(jnp.sum(values, axis=1), "cb")
    mean = total / width
    centred = values - mean[:, None]
    spread = lax.psum(jnp.sum(centred * centred, axis=1), "cb") / width
    return centred * lax.rsqrt(spread + EPS)[:, None]


def plain(
    tokens,
    norm_gain,
    norm_bias,
    gate_weight,
    up_weight,
    gate_scale,
    up_scale,
    down_weight,
    down_scale,
    out_gain,
    out_bias,
):
    normed = (standardize(tokens.astype(F32)) * norm_gain + norm_bias).astype(BF16)
    gate_part = jnp.dot(normed, gate_weight.astype(BF16), preferred_element_type=F32)
    up_part = jnp.dot(normed, up_weight.astype(BF16), preferred_element_type=F32)
    gate_share, up_share = (
        lax.psum_scatter(part.astype(BF16), "cb", scatter_dimension=1, tiled=True).astype(F32)
        for part in (gate_part, up_part)
    )
    share = gate_share.shape[1]
    offset = lax.axis_index("cb") * share
    gate_cols = lax.dynamic_slice_in_dim(gate_scale, offset, share, 0)
    up_cols = lax.dynamic_slice_in_dim(up_scale, offset, share, 0)
    hidden_share = (jax.nn.silu(gate_share * gate_cols) * (up_share * up_cols)).astype(BF16)
    hidden = lax.all_gather(hidden_share, "cb", axis=1, tiled=True)
    own_rows = hidden.shape[0] // lax.axis_size("ra")
    part = jnp.dot(hidden, down_weight.astype(BF16), preferred_element_type=F32)
    branch = lax.psum_scatter(part, "ra", scatter_dimension=0, tiled=True) * down_scale
    own_normed = lax.dynamic_slice_in_dim(normed, lax.axis_index("ra") * own_rows, own_rows, 0)
    mixed = 0.5 * own_normed.astype(F32) + branch
    return (standardize(mixed) * out_gain + out_bias).astype(BF16)


S1, S2, S3, S4, S5, WD = range(6)
ORDER = (
    (S1, 0), (S1, 1), (WD, 0), (S2, 0), (S2, 1), (S3, 0), (S1, 2), (S3, 1), (S4, 0), (S2, 2), (S4, 1),
    (S5, 0), (S1, 3), (S3, 2), (S5, 1), (S2, 3), (S4, 2), (S3, 3), (S5, 2), (S4, 3), (S5, 3),
)


def kernel(
    tok,
    ng,
    nb,
    gw,
    uw,
    gs,
    us,
    dw,
    down_scale,
    og,
    ob,
    out,
    stage,
    stage_d,
    wg,
    wu,
    wd,
    nrm,
    pg,
    pu,
    r1g,
    r1u,
    rdg,
    r2g,
    rdu,
    r2u,
    hid,
    bp,
    zr,
    mix,
    st,
    st2,
    stage_sem,
    stage_d_sem,
    send,
    recv,
    st_send,
    st_recv,
):
    rows, width = tok.shape
    ff = wg.shape[1]
    tiles = ff // TILE
    blk = rows // (G * G)
    chunk = G * blk
    full = float(width * G)

    b = lax.axis_index("cb")
    r = lax.axis_index("ra")
    xn = b + 1 - 2 * lax.rem(b, 2)
    yn = lax.rem(b + 2, G)
    dg = (G - 1) - b
    zs = [lax.rem(r + o, G) for o in range(1, G)]

    def to(axis, index):
        return {axis: index}

    peers = [to("cb", xn), to("cb", yn), to("cb", dg)] + [to("ra", z) for z in zs]
    barrier = pltpu.get_barrier_semaphore()
    for peer in peers:
        pl.semaphore_signal(barrier, inc=1, device_id=peer, device_id_type=MESH)

    def tile_cols(t):
        return pl.ds(pl.multiple_of(t * TILE, TILE), TILE)

    def load_gu(t, slot):
        return (
            pltpu.make_async_copy(gw.at[:, tile_cols(t)], stage.at[slot], stage_sem.at[slot]),
            pltpu.make_async_copy(uw.at[:, tile_cols(t)], stage.at[2 + slot], stage_sem.at[2 + slot]),
        )

    for t in range(2):
        for copy in load_gu(t, t):
            copy.start()

    def put_stats(x, dst, col):
        total = jnp.sum(x, axis=1, keepdims=True)
        off = x - total * (1.0 / width)
        spread = jnp.sum(off * off, axis=1, keepdims=True)
        lane = lax.broadcasted_iota(jnp.int32, (x.shape[0], 128), 1)
        both = jnp.where(lane == 0, total, spread)
        dst[0, :, pl.ds(col, x.shape[0])] = both.T[:8, :]

    def get_stats(src, col, n):
        parts = [src[i, 0:2, pl.ds(col, n)] for i in range(G)]
        mean = (parts[0][0:1] + parts[1][0:1] + parts[2][0:1] + parts[3][0:1]) / full
        spread = jnp.zeros_like(mean)
        for p in parts:
            d = p[0:1] * (1.0 / width) - mean
            spread = spread + p[1:2] + width * (d * d)
        inv = lax.rsqrt(spread / full + EPS)
        sub = lax.broadcasted_iota(jnp.int32, (128, n), 0)
        both = jnp.where(sub == 0, mean, inv).T
        return both[:, 0:1], both[:, 1:2]

    def swap_stats(buf, which):
        copies = []
        for i, peer in enumerate(peers[:3]):
            copies.append(
                pltpu.make_async_remote_copy(
                    src_ref=buf.at[0],
                    dst_ref=buf.at[1 + i],
                    send_sem=st_send.at[which, i],
                    recv_sem=st_recv.at[which, i],
                    device_id=peer,
                    device_id_type=MESH,
                )
            )
        return copies

    for j in range(G):
        put_stats(tok[pl.ds(j * chunk, chunk), :].astype(F32), st, j * chunk)

    pl.semaphore_wait(barrier, len(peers))
    swap1 = swap_stats(st, 0)
    for copy in swap1:
        copy.start()

    def cast_gu(t, carry):
        slot = lax.rem(t, 2)
        for copy in load_gu(t, slot):
            copy.wait()
        wg[:, tile_cols(t)] = stage[slot].astype(BF16)
        wu[:, tile_cols(t)] = stage[2 + slot].astype(BF16)

        @pl.when(t + 2 < tiles)
        def _():
            for copy in load_gu(t + 2, slot):
                copy.start()

        return carry

    lax.fori_loop(0, tiles, cast_gu, 0)

    def tile_rows(t):
        return pl.ds(pl.multiple_of(t * TILE, TILE), TILE)

    def load_d(t, slot):
        return pltpu.make_async_copy(dw.at[tile_rows(t), :], stage_d.at[slot], stage_d_sem.at[slot])

    for t in range(2):
        load_d(t, t).start()

    for copy in swap1:
        copy.wait_recv()
    for j in range(G):
        mean, inv = get_stats(st, j * chunk, chunk)
        x = tok[pl.ds(j * chunk, chunk), :].astype(F32)
        y = ((x - mean) * inv * ng[...] + nb[...]).astype(BF16)
        for c in range(G):
            nrm[c, pl.ds(j * blk, blk), :] = y[c * blk : (c + 1) * blk, :]

    def remote(kind, c, src, dst, peer):
        return pltpu.make_async_remote_copy(
            src_ref=src,
            dst_ref=dst,
            send_sem=send.at[kind, c],
            recv_sem=recv.at[kind, c],
            device_id=peer,
            device_id_type=MESH,
        )

    px, py = peers[0], peers[1]
    half = ff // 2 // 128 * 128
    cp = {}
    for c in range(G):
        mine = pl.ds(pl.multiple_of(b * blk, blk), blk)
        of_x = pl.ds(pl.multiple_of(xn * blk, blk), blk)
        of_y = pl.ds(pl.multiple_of(yn * blk, blk), blk)
        lo, hi = pl.ds(0, half), pl.ds(half, ff - half)
        cp[c] = [
            remote(0, c, pg.at[c, dg], r1g.at[c], px),
            remote(1, c, pu.at[c, dg], r1u.at[c], py),
            remote(2, c, pg.at[c, xn], rdg.at[c], px),
            remote(3, c, pu.at[c, yn], rdu.at[c], py),
            remote(4, c, pg.at[c, yn], r2g.at[c], py),
            remote(5, c, pu.at[c, xn], r2u.at[c], px),
            remote(6, c, hid.at[c, mine], hid.at[c, mine], px),
            remote(7, c, hid.at[c, mine], hid.at[c, mine], py),
            remote(8, c, hid.at[c, of_x, lo], hid.at[c, of_x, lo], py),
            remote(9, c, hid.at[c, of_y, hi], hid.at[c, of_y, hi], px),
        ]
        for o, z in enumerate(zs):
            rowz = pl.ds(pl.multiple_of(z * blk, blk), blk)
            cp[c].append(remote(10 + o, c, bp.at[c, rowz], zr.at[c, o], peers[3 + o]))

    def s1(c):
        def body(t, carry):
            cols = tile_cols(t)
            x = nrm[c]
            g = jnp.dot(x, wg[:, cols], preferred_element_type=F32).astype(BF16)
            u = jnp.dot(x, wu[:, cols], preferred_element_type=F32).astype(BF16)
            for j in range(G):
                pg[c, j, :, cols] = g[j * blk : (j + 1) * blk, :]
                pu[c, j, :, cols] = u[j * blk : (j + 1) * blk, :]
            return carry

        lax.fori_loop(0, tiles, body, 0)
        for k in range(4):
            cp[c][k].start()

    def w_down(_):
        def body(t, carry):
            slot = lax.rem(t, 2)
            load_d(t, slot).wait()
            wd[tile_rows(t), :] = stage_d[slot].astype(BF16)

            @pl.when(t + 2 < tiles)
            def _():
                load_d(t + 2, slot).start()

            return carry

        lax.fori_loop(0, tiles, body, 0)

    def s2(c):
        cp[c][0].wait_recv()
        cp[c][1].wait_recv()

        def body(t, carry):
            cols = tile_cols(t)
            pg[c, yn, :, cols] = (pg[c, yn, :, cols].astype(F32) + r1g[c, :, cols].astype(F32)).astype(BF16)
            pu[c, xn, :, cols] = (pu[c, xn, :, cols].astype(F32) + r1u[c, :, cols].astype(F32)).astype(BF16)
            return carry

        lax.fori_loop(0, tiles, body, 0)
        cp[c][4].start()
        cp[c][5].start()

    def s3(c):
        for k in range(2, 6):
            cp[c][k].wait_recv()

        def body(t, carry):
            cols = tile_cols(t)
            g = pg[c, b, :, cols].astype(F32) + rdg[c, :, cols].astype(F32) + r2g[c, :, cols].astype(F32)
            u = pu[c, b, :, cols].astype(F32) + rdu[c, :, cols].astype(F32) + r2u[c, :, cols].astype(F32)
            g = g * gs[:, cols]
            u = u * us[:, cols]
            h = (g / (1.0 + jnp.exp(-g)) * u).astype(BF16)
            hid[c, pl.ds(pl.multiple_of(b * blk, blk), blk), cols] = h
            return carry

        lax.fori_loop(0, tiles, body, 0)
        cp[c][6].start()
        cp[c][7].start()

    def s4(c):
        cp[c][6].wait_recv()
        cp[c][8].start()
        cp[c][7].wait_recv()
        cp[c][9].start()

    def s5(c):
        cp[c][8].wait_recv()
        cp[c][9].wait_recv()

        def body(t, carry):
            cols = tile_cols(t)
            bp[c, :, cols] = jnp.dot(hid[c], wd[:, cols], preferred_element_type=F32).astype(BF16)
            return carry

        lax.fori_loop(0, width // TILE, body, 0)
        for o in (1, 0, 2):
            cp[c][10 + o].start()

    steps = (s1, s2, s3, s4, s5, w_down)
    for step, c in ORDER:
        steps[step](c)

    mine = pl.ds(pl.multiple_of(r * blk, blk), blk)
    for c in range(G):
        for o in (1, 0, 2):
            cp[c][10 + o].wait_recv()
        total = bp[c, mine, :].astype(F32)
        for o in range(G - 1):
            total = total + zr[c, o].astype(F32)
        mix[pl.ds(c * blk, blk), :] = 0.5 * nrm[c, mine, :].astype(F32) + total * down_scale[...]
    put_stats(mix[...], st2, 0)
    swap2 = swap_stats(st2, 1)
    for copy in swap2:
        copy.start()
    for copy in swap2:
        copy.wait_recv()
    mean, inv = get_stats(st2, 0, chunk)
    out[...] = ((mix[...] - mean) * inv * og[...] + ob[...]).astype(BF16)

    for copy in swap1 + swap2:
        copy.wait_send()
    for c in range(G):
        for copy in cp[c]:
            copy.wait_send()


def fused(
    tokens,
    norm_gain,
    norm_bias,
    gate_weight,
    up_weight,
    gate_scale,
    up_scale,
    down_weight,
    down_scale,
    out_gain,
    out_bias,
):
    rows, width = tokens.shape
    ff = gate_weight.shape[1]
    blk = rows // (G * G)
    chunk = G * blk
    vmem = pl.BlockSpec(memory_space=pltpu.VMEM)
    hbm = pl.BlockSpec(memory_space=pl.ANY)
    block = pltpu.VMEM((G, blk, ff), BF16)
    row = lambda v: v.reshape(1, -1)
    return pl.pallas_call(
        kernel,
        out_shape=jax.ShapeDtypeStruct((chunk, width), BF16),
        in_specs=[vmem, vmem, vmem, hbm, hbm, vmem, vmem, hbm, vmem, vmem, vmem],
        out_specs=vmem,
        scratch_shapes=[
            pltpu.VMEM((4, width, TILE), F32),
            pltpu.VMEM((2, TILE, width), F32),
            pltpu.VMEM((width, ff), BF16),
            pltpu.VMEM((width, ff), BF16),
            pltpu.VMEM((ff, width), BF16),
            pltpu.VMEM((G, chunk, width), BF16),
            pltpu.VMEM((G, G, blk, ff), BF16),
            pltpu.VMEM((G, G, blk, ff), BF16),
            block,
            block,
            block,
            block,
            block,
            block,
            pltpu.VMEM((G, chunk, ff), BF16),
            pltpu.VMEM((G, chunk, width), BF16),
            pltpu.VMEM((G, G - 1, blk, width), BF16),
            pltpu.VMEM((chunk, width), F32),
            pltpu.VMEM((G, 8, rows), F32),
            pltpu.VMEM((G, 8, chunk), F32),
            pltpu.SemaphoreType.DMA((4,)),
            pltpu.SemaphoreType.DMA((2,)),
            pltpu.SemaphoreType.DMA((13, G)),
            pltpu.SemaphoreType.DMA((13, G)),
            pltpu.SemaphoreType.DMA((2, G - 1)),
            pltpu.SemaphoreType.DMA((2, G - 1)),
        ],
        compiler_params=pltpu.CompilerParams(
            collective_id=0, has_side_effects=True, vmem_limit_bytes=67043328
        ),
    )(
        tokens,
        row(norm_gain),
        row(norm_bias),
        gate_weight,
        up_weight,
        row(gate_scale),
        row(up_scale),
        down_weight,
        row(down_scale),
        row(out_gain),
        row(out_bias),
    )


def local(*args):
    rows, width = args[0].shape
    ff = args[3].shape[1]
    fits = (
        lax.axis_size("cb") == G
        and lax.axis_size("ra") == G
        and rows % (16 * G * G) == 0
        and width % TILE == 0
        and ff % TILE == 0
        and rows * width <= 1 << 20
        and ff * width <= 2816 * 1024
    )
    return (fused if fits else plain)(*args)


def solution(mesh):
    return jax.shard_map(
        local,
        mesh=mesh,
        in_specs=(
            P("dp", "cb"),
            P("cb"),
            P("cb"),
            P("cb", "ra"),
            P("cb", "ra"),
            P("ra"),
            P("ra"),
            P("ra", "cb"),
            P("cb"),
            P("cb"),
            P("cb"),
        ),
        out_specs=P(("dp", "ra"), "cb"),
        check_vma=False,
    )
```

```python
import jax
import jax.numpy as jnp
from jax import lax
from jax.experimental import pallas as pl
from jax.experimental.pallas import tpu as pltpu
from jax.sharding import PartitionSpec as P

MESH = pl.DeviceIdType.MESH
EPS = 1e-05
TILE = 256
G = 4
F32 = jnp.float32
BF16 = jnp.bfloat16


def standardize(values):
    width = values.shape[1] * lax.axis_size("cb")
    total = lax.psum(jnp.sum(values, axis=1), "cb")
    mean = total / width
    centred = values - mean[:, None]
    spread = lax.psum(jnp.sum(centred * centred, axis=1), "cb") / width
    return centred * lax.rsqrt(spread + EPS)[:, None]


def plain(
    tokens,
    norm_gain,
    norm_bias,
    gate_weight,
    up_weight,
    gate_scale,
    up_scale,
    down_weight,
    down_scale,
    out_gain,
    out_bias,
):
    normed = (standardize(tokens.astype(F32)) * norm_gain + norm_bias).astype(BF16)
    gate_part = jnp.dot(normed, gate_weight.astype(BF16), preferred_element_type=F32)
    up_part = jnp.dot(normed, up_weight.astype(BF16), preferred_element_type=F32)
    gate_share, up_share = (
        lax.psum_scatter(part.astype(BF16), "cb", scatter_dimension=1, tiled=True).astype(F32)
        for part in (gate_part, up_part)
    )
    share = gate_share.shape[1]
    offset = lax.axis_index("cb") * share
    gate_cols = lax.dynamic_slice_in_dim(gate_scale, offset, share, 0)
    up_cols = lax.dynamic_slice_in_dim(up_scale, offset, share, 0)
    hidden_share = (jax.nn.silu(gate_share * gate_cols) * (up_share * up_cols)).astype(BF16)
    hidden = lax.all_gather(hidden_share, "cb", axis=1, tiled=True)
    own_rows = hidden.shape[0] // lax.axis_size("ra")
    part = jnp.dot(hidden, down_weight.astype(BF16), preferred_element_type=F32)
    branch = lax.psum_scatter(part, "ra", scatter_dimension=0, tiled=True) * down_scale
    own_normed = lax.dynamic_slice_in_dim(normed, lax.axis_index("ra") * own_rows, own_rows, 0)
    mixed = 0.5 * own_normed.astype(F32) + branch
    return (standardize(mixed) * out_gain + out_bias).astype(BF16)


NC = 8
SKEW = (0, 1, 2, 3, 4)


def schedule():
    steps = []
    for t in range(NC + max(SKEW)):
        for stage, behind in enumerate(SKEW):
            if 0 <= t - behind < NC:
                steps.append((stage, t - behind))
    return steps


def kernel(
    tok,
    ng,
    nb,
    gw,
    uw,
    gs,
    us,
    dw,
    down_scale,
    og,
    ob,
    out,
    stage,
    stage_d,
    wg,
    wu,
    wd,
    nrm,
    pg,
    pu,
    r1g,
    r1u,
    rdg,
    r2g,
    rdu,
    r2u,
    hid,
    bp,
    zr,
    mix,
    st,
    st2,
    stage_sem,
    stage_d_sem,
    send,
    recv,
    st_send,
    st_recv,
):
    rows, width = tok.shape
    ff = wg.shape[1]
    tiles = ff // TILE
    blk = rows // (G * NC)
    chunk = G * blk
    part = rows // G
    full = float(width * G)

    b = lax.axis_index("cb")
    r = lax.axis_index("ra")
    xn = b + 1 - 2 * lax.rem(b, 2)
    yn = lax.rem(b + 2, G)
    dg = (G - 1) - b
    zs = [lax.rem(r + o, G) for o in range(1, G)]

    def to(axis, index):
        return {axis: index}

    peers = [to("cb", xn), to("cb", yn), to("cb", dg)] + [to("ra", z) for z in zs]
    barrier = pltpu.get_barrier_semaphore()
    for peer in peers:
        pl.semaphore_signal(barrier, inc=1, device_id=peer, device_id_type=MESH)

    def tile_cols(t):
        return pl.ds(pl.multiple_of(t * TILE, TILE), TILE)

    def load_gu(t, slot):
        return (
            pltpu.make_async_copy(gw.at[:, tile_cols(t)], stage.at[slot], stage_sem.at[slot]),
            pltpu.make_async_copy(uw.at[:, tile_cols(t)], stage.at[2 + slot], stage_sem.at[2 + slot]),
        )

    for t in range(2):
        for copy in load_gu(t, t):
            copy.start()

    def put_stats(x, dst, col):
        total = jnp.sum(x, axis=1, keepdims=True)
        off = x - total * (1.0 / width)
        spread = jnp.sum(off * off, axis=1, keepdims=True)
        lane = lax.broadcasted_iota(jnp.int32, (x.shape[0], 128), 1)
        both = jnp.where(lane == 0, total, spread)
        dst[0, :, pl.ds(col, x.shape[0])] = both.T[:8, :]

    def get_stats(src, col, n):
        parts = [src[i, 0:2, pl.ds(col, n)] for i in range(G)]
        mean = (parts[0][0:1] + parts[1][0:1] + parts[2][0:1] + parts[3][0:1]) / full
        spread = jnp.zeros_like(mean)
        for p in parts:
            d = p[0:1] * (1.0 / width) - mean
            spread = spread + p[1:2] + width * (d * d)
        inv = lax.rsqrt(spread / full + EPS)
        sub = lax.broadcasted_iota(jnp.int32, (128, n), 0)
        both = jnp.where(sub == 0, mean, inv).T
        return both[:, 0:1], both[:, 1:2]

    def swap_stats(buf, which):
        copies = []
        for i, peer in enumerate(peers[:3]):
            copies.append(
                pltpu.make_async_remote_copy(
                    src_ref=buf.at[0],
                    dst_ref=buf.at[1 + i],
                    send_sem=st_send.at[which, i],
                    recv_sem=st_recv.at[which, i],
                    device_id=peer,
                    device_id_type=MESH,
                )
            )
        return copies

    for j in range(G):
        put_stats(tok[pl.ds(j * part, part), :].astype(F32), st, j * part)

    pl.semaphore_wait(barrier, len(peers))
    swap1 = swap_stats(st, 0)
    for copy in swap1:
        copy.start()

    def cast_gu(t, carry):
        slot = lax.rem(t, 2)
        for copy in load_gu(t, slot):
            copy.wait()
        wg[:, tile_cols(t)] = stage[slot].astype(BF16)
        wu[:, tile_cols(t)] = stage[2 + slot].astype(BF16)

        @pl.when(t + 2 < tiles)
        def _():
            for copy in load_gu(t + 2, slot):
                copy.start()

        return carry

    lax.fori_loop(0, tiles, cast_gu, 0)

    def tile_rows(t):
        return pl.ds(pl.multiple_of(t * TILE, TILE), TILE)

    def load_d(t, slot):
        return pltpu.make_async_copy(dw.at[tile_rows(t), :], stage_d.at[slot], stage_d_sem.at[slot])

    for t in range(2):
        load_d(t, t).start()

    for copy in swap1:
        copy.wait_recv()
    for j in range(G):
        mean, inv = get_stats(st, j * part, part)
        x = tok[pl.ds(j * part, part), :].astype(F32)
        y = ((x - mean) * inv * ng[...] + nb[...]).astype(BF16)
        for c in range(NC):
            nrm[c, pl.ds(j * blk, blk), :] = y[c * blk : (c + 1) * blk, :]

    def remote(kind, c, src, dst, peer):
        return pltpu.make_async_remote_copy(
            src_ref=src,
            dst_ref=dst,
            send_sem=send.at[kind, c],
            recv_sem=recv.at[kind, c],
            device_id=peer,
            device_id_type=MESH,
        )

    px, py = peers[0], peers[1]
    half = ff // 2 // 128 * 128
    cp = {}
    for c in range(NC):
        mine = pl.ds(pl.multiple_of(b * blk, blk), blk)
        of_x = pl.ds(pl.multiple_of(xn * blk, blk), blk)
        of_y = pl.ds(pl.multiple_of(yn * blk, blk), blk)
        lo, hi = pl.ds(0, half), pl.ds(half, ff - half)
        cp[c] = [
            remote(0, c, pg.at[c, dg], r1g.at[c], px),
            remote(1, c, pu.at[c, dg], r1u.at[c], py),
            remote(2, c, pg.at[c, xn], rdg.at[c], px),
            remote(3, c, pu.at[c, yn], rdu.at[c], py),
            remote(4, c, pg.at[c, yn], r2g.at[c], py),
            remote(5, c, pu.at[c, xn], r2u.at[c], px),
            remote(6, c, hid.at[c, mine], hid.at[c, mine], px),
            remote(7, c, hid.at[c, mine], hid.at[c, mine], py),
            remote(8, c, hid.at[c, of_x, lo], hid.at[c, of_x, lo], py),
            remote(9, c, hid.at[c, of_y, hi], hid.at[c, of_y, hi], px),
        ]
        for o, z in enumerate(zs):
            rowz = pl.ds(pl.multiple_of(z * blk, blk), blk)
            cp[c].append(remote(10 + o, c, bp.at[c, rowz], zr.at[c, o], peers[3 + o]))

    def s1(c):
        def body(t, carry):
            cols = tile_cols(t)
            x = nrm[c]
            g = jnp.dot(x, wg[:, cols], preferred_element_type=F32).astype(BF16)
            u = jnp.dot(x, wu[:, cols], preferred_element_type=F32).astype(BF16)
            for j in range(G):
                pg[c, j, :, cols] = g[j * blk : (j + 1) * blk, :]
                pu[c, j, :, cols] = u[j * blk : (j + 1) * blk, :]
            return carry

        lax.fori_loop(0, tiles, body, 0)
        for k in range(4):
            cp[c][k].start()

    def w_down(_):
        def body(t, carry):
            slot = lax.rem(t, 2)
            load_d(t, slot).wait()
            wd[tile_rows(t), :] = stage_d[slot].astype(BF16)

            @pl.when(t + 2 < tiles)
            def _():
                load_d(t + 2, slot).start()

            return carry

        lax.fori_loop(0, tiles, body, 0)

    def s2(c):
        cp[c][0].wait_recv()
        cp[c][1].wait_recv()

        def body(t, carry):
            cols = tile_cols(t)
            pg[c, yn, :, cols] = (pg[c, yn, :, cols].astype(F32) + r1g[c, :, cols].astype(F32)).astype(BF16)
            pu[c, xn, :, cols] = (pu[c, xn, :, cols].astype(F32) + r1u[c, :, cols].astype(F32)).astype(BF16)
            return carry

        lax.fori_loop(0, tiles, body, 0)
        cp[c][4].start()
        cp[c][5].start()

    def s3(c):
        for k in range(2, 6):
            cp[c][k].wait_recv()

        def body(t, carry):
            cols = tile_cols(t)
            g = pg[c, b, :, cols].astype(F32) + rdg[c, :, cols].astype(F32) + r2g[c, :, cols].astype(F32)
            u = pu[c, b, :, cols].astype(F32) + rdu[c, :, cols].astype(F32) + r2u[c, :, cols].astype(F32)
            g = g * gs[:, cols]
            u = u * us[:, cols]
            h = (g / (1.0 + jnp.exp(-g)) * u).astype(BF16)
            hid[c, pl.ds(pl.multiple_of(b * blk, blk), blk), cols] = h
            return carry

        lax.fori_loop(0, tiles, body, 0)
        cp[c][6].start()
        cp[c][7].start()

    def s4(c):
        cp[c][6].wait_recv()
        cp[c][8].start()
        cp[c][7].wait_recv()
        cp[c][9].start()

    def s5(c):
        cp[c][8].wait_recv()
        cp[c][9].wait_recv()

        def body(t, carry):
            cols = tile_cols(t)
            bp[c, :, cols] = jnp.dot(hid[c], wd[:, cols], preferred_element_type=F32).astype(BF16)
            return carry

        lax.fori_loop(0, width // TILE, body, 0)
        for o in (1, 0, 2):
            cp[c][10 + o].start()

    steps = (s1, s2, s3, s4, s5)
    for i, (step, c) in enumerate(schedule()):
        if i == 2:
            w_down(0)
        steps[step](c)

    mine = pl.ds(pl.multiple_of(r * blk, blk), blk)
    for c in range(NC):
        for o in (1, 0, 2):
            cp[c][10 + o].wait_recv()
        total = bp[c, mine, :].astype(F32)
        for o in range(G - 1):
            total = total + zr[c, o].astype(F32)
        mix[pl.ds(c * blk, blk), :] = 0.5 * nrm[c, mine, :].astype(F32) + total * down_scale[...]
    put_stats(mix[...], st2, 0)
    swap2 = swap_stats(st2, 1)
    for copy in swap2:
        copy.start()
    for copy in swap2:
        copy.wait_recv()
    mean, inv = get_stats(st2, 0, part)
    out[...] = ((mix[...] - mean) * inv * og[...] + ob[...]).astype(BF16)

    for copy in swap1 + swap2:
        copy.wait_send()
    for c in range(NC):
        for copy in cp[c]:
            copy.wait_send()


def fused(
    tokens,
    norm_gain,
    norm_bias,
    gate_weight,
    up_weight,
    gate_scale,
    up_scale,
    down_weight,
    down_scale,
    out_gain,
    out_bias,
):
    rows, width = tokens.shape
    ff = gate_weight.shape[1]
    blk = rows // (G * NC)
    chunk = G * blk
    part = rows // G
    vmem = pl.BlockSpec(memory_space=pltpu.VMEM)
    hbm = pl.BlockSpec(memory_space=pl.ANY)
    block = pltpu.VMEM((NC, blk, ff), BF16)
    row = lambda v: v.reshape(1, -1)
    return pl.pallas_call(
        kernel,
        out_shape=jax.ShapeDtypeStruct((part, width), BF16),
        in_specs=[vmem, vmem, vmem, hbm, hbm, vmem, vmem, hbm, vmem, vmem, vmem],
        out_specs=vmem,
        scratch_shapes=[
            pltpu.VMEM((4, width, TILE), F32),
            pltpu.VMEM((2, TILE, width), F32),
            pltpu.VMEM((width, ff), BF16),
            pltpu.VMEM((width, ff), BF16),
            pltpu.VMEM((ff, width), BF16),
            pltpu.VMEM((NC, chunk, width), BF16),
            pltpu.VMEM((NC, G, blk, ff), BF16),
            pltpu.VMEM((NC, G, blk, ff), BF16),
            block,
            block,
            block,
            block,
            block,
            block,
            pltpu.VMEM((NC, chunk, ff), BF16),
            pltpu.VMEM((NC, chunk, width), BF16),
            pltpu.VMEM((NC, G - 1, blk, width), BF16),
            pltpu.VMEM((part, width), F32),
            pltpu.VMEM((G, 8, rows), F32),
            pltpu.VMEM((G, 8, part), F32),
            pltpu.SemaphoreType.DMA((4,)),
            pltpu.SemaphoreType.DMA((2,)),
            pltpu.SemaphoreType.DMA((13, NC)),
            pltpu.SemaphoreType.DMA((13, NC)),
            pltpu.SemaphoreType.DMA((2, G - 1)),
            pltpu.SemaphoreType.DMA((2, G - 1)),
        ],
        compiler_params=pltpu.CompilerParams(
            collective_id=0, has_side_effects=True, vmem_limit_bytes=67043328
        ),
    )(
        tokens,
        row(norm_gain),
        row(norm_bias),
        gate_weight,
        up_weight,
        row(gate_scale),
        row(up_scale),
        down_weight,
        row(down_scale),
        row(out_gain),
        row(out_bias),
    )


def local(*args):
    rows, width = args[0].shape
    ff = args[3].shape[1]
    fits = (
        lax.axis_size("cb") == G
        and lax.axis_size("ra") == G
        and rows % (16 * G * NC) == 0
        and rows % (128 * G) == 0
        and width % TILE == 0
        and ff % TILE == 0
        and rows * width <= 1 << 20
        and ff * width <= 2816 * 1024
    )
    return (fused if fits else plain)(*args)


def solution(mesh):
    return jax.shard_map(
        local,
        mesh=mesh,
        in_specs=(
            P("dp", "cb"),
            P("cb"),
            P("cb"),
            P("cb", "ra"),
            P("cb", "ra"),
            P("ra"),
            P("ra"),
            P("ra", "cb"),
            P("cb"),
            P("cb"),
            P("cb"),
        ),
        out_specs=P(("dp", "ra"), "cb"),
        check_vma=False,
    )
```
